32 devices in a mesh: sp: 8 (over z, x), tp: 4 (over y, core).
Axes of the slice: x: 2, y: 2, z: 4, core: 2. Of those that a mesh axis runs over, the one named last changes fastest.
Arguments:
- residual_matrix: bfloat16 [2048, 2048], P(('sp', 'tp')), may hold values from -6 to 6
- query_vectors: bfloat16 [2048, 2048], P('tp', 'sp'), may hold values from -6 to 6
- lookup_vectors: bfloat16 [2048, 2048], P('tp', 'sp'), may hold values from -6 to 6
- payload_vectors: bfloat16 [2048, 2048], P('tp', 'sp'), may hold values from -6 to 6
- fading_dependent_term: bfloat16 [2048, 2048], P('tp', 'sp'), may hold values from -4 to 4
- step_size_preactivation: bfloat16 [2048, 2048], P('tp', 'sp'), may hold values from -8 to 8
- attention_result_switch: bfloat16 [2048, 2048], P('tp', 'sp'), may hold values from -6 to 6
- fading_bias_vector: float32 [2048], P('tp'), may hold values from -16 to -2
- surplus_forgetting: float32 [32, 2048], P('tp', 'sp'), may hold values from -0.7 to 0
- per_group_scaler: float32 [2048], P('tp'), may hold values from 0.1 to 1.9
- attention_result_matrix: bfloat16 [2048, 2048], P('tp'), may hold values from -0.125 to 0.125
- dense_block_scaler: float32 [2048], replicated, may hold values from 0.1 to 1.9
- switching_matrix: bfloat16 [2048, 5632], P('sp', 'tp'), may hold values from -0.125 to 0.125
- expanding_matrix: bfloat16 [2048, 5632], P('sp', 'tp'), may hold values from -0.125 to 0.125
- contracting_matrix: bfloat16 [5632, 2048], P('tp', 'sp'), may hold values from -0.078125 to 0.078125
Outputs:
- blended: bfloat16 [2048, 2048], P(('sp', 'tp'))
The draws below stay inside these ranges and needn't reach their ends.
All inputs are finite; a program needn't handle non-finite values.
Results may differ from the reference program's by a relative error of at most 0.015.
Values may be sent and summed in bfloat16 or wider, within the bound.
A program may use at most 128 MiB of HBM per device.

```python
import math
import jax
import jax.numpy as jnp
from jax import lax

D = 2048
HEAD = 64
HEADS = 32
FF = 5632
BLOCK = 64
TOK_DEV = 256
MIX = 2048
TOKENS = 2048
N_TP = 4


def draw_lookup_vectors(key, part):
    noise_key = jax.random.fold_in(key, 41)
    quiet_key = jax.random.fold_in(key, 42)
    level_key = jax.random.fold_in(key, 43)
    direction_key = jax.random.fold_in(key, 44)
    block_key = jax.random.fold_in(key, 45)
    noise = jnp.clip(jax.random.normal(noise_key, (HEADS, HEAD, TOKENS), jnp.float32), -5.0, 5.0)
    quiet = jax.random.uniform(quiet_key, (HEADS, HEAD, 1), jnp.float32) < 0.25
    quiet_level = jnp.exp(jax.random.uniform(level_key, (HEADS, HEAD, 1), jnp.float32, math.log(0.01), math.log(0.05)))
    position = jnp.arange(TOKENS)[None, None, :]
    later = position >= TOK_DEV
    factor = jnp.where(jnp.logical_and(quiet, later), quiet_level, 1.0)
    direction = jax.random.normal(direction_key, (HEADS, HEAD, 1), jnp.float32)
    direction = direction * (3.0 / jnp.sqrt(jnp.sum(direction * direction, axis=1, keepdims=True) + 1e-06))
    chosen = jax.random.uniform(block_key, (HEADS, 1, TOKENS // BLOCK), jnp.float32) < 0.25
    chosen = jnp.repeat(chosen, BLOCK, axis=2)
    keys = (noise + jnp.where(chosen, direction, 0.0)) * factor
    return jnp.clip(keys, -6.0, 6.0).reshape(MIX, TOKENS).astype(jnp.bfloat16)


def draw_fading_bias_vector(key, part):
    first_key = jax.random.fold_in(key, 11)
    second_key = jax.random.fold_in(key, 12)
    fast_share = 0.5
    fast_heads = jax.random.uniform(first_key, (HEADS, 1), jnp.float32) < fast_share
    jitter = jax.random.uniform(second_key, (HEADS, HEAD), jnp.float32, -0.5, 0.5)
    slow_level = math.log(0.6 / TOKENS) + 0.5
    return (jnp.where(fast_heads, -3.4, slow_level) + jitter).reshape(HEADS * HEAD).astype(jnp.float32)


def draw_fading_dependent_term(key, part):
    first_key = jax.random.fold_in(key, 21)
    second_key = jax.random.fold_in(key, 22)
    noise = jnp.clip(jax.random.normal(first_key, (MIX, TOKENS), jnp.float32) * 0.7, -3.0, 3.0)
    levels = jax.random.uniform(second_key, (TOKENS // TOK_DEV,), jnp.float32, -0.7, 0.7)
    return (noise + jnp.repeat(levels, TOK_DEV)[None, :]).astype(jnp.bfloat16)


def draw_surplus_forgetting(key, part):
    first_key = jax.random.fold_in(key, 31)
    second_key = jax.random.fold_in(key, 32)
    struck = jax.random.uniform(first_key, (HEADS, TOKENS), jnp.float32) < 3.0 / TOKENS
    losses = jnp.log(jax.random.uniform(second_key, (HEADS, TOKENS), jnp.float32, 0.5, 0.8))
    return jnp.where(struck, losses, 0.0).astype(jnp.float32)


def shard_levels(own_key, extent, shards, smallest, high):
    factor_of = 1.0
    for dim, shards_of in shards:
        heights = jax.random.uniform(jax.random.fold_in(jax.random.fold_in(own_key, 6), dim), (shards_of,), jnp.float32, smallest / len(shards), high / len(shards))
        factor_of = factor_of * jnp.repeat(jnp.exp(heights), extent[dim] // shards_of).reshape((-1,) + (1,) * (len(extent) - 1 - dim))
    return factor_of


def bell_draw(key, extent, spread, limit, split=(), kind=jnp.bfloat16):
    entries = spread * jax.random.normal(key, extent, jnp.float32)
    if split:
        entries = entries * shard_levels(key, extent, split, -0.22, 0.18)
    return jnp.clip(entries, -limit, limit).astype(kind)


def setup_inputs(seed: int = 0) -> dict:
    streams_of = jax.random.split(jax.random.key(seed), 16)
    residual_matrix = bell_draw(streams_of[0], (TOKENS, D), 1.0, 6.0, ((0, 32),))
    query_vectors = bell_draw(streams_of[1], (MIX, TOKENS), 1.0, 6.0, ((0, 4), (1, 8)))
    lookup_vectors = draw_lookup_vectors(jax.random.fold_in(streams_of[15], 71), 0)
    payload_vectors = bell_draw(streams_of[3], (MIX, TOKENS), 1.0, 6.0, ((0, 4), (1, 8)))
    fading_dependent_term = draw_fading_dependent_term(jax.random.fold_in(streams_of[15], 71), 0)
    step_size_preactivation = bell_draw(streams_of[5], (MIX, TOKENS), 1.5, 8.0, ((0, 4), (1, 8)))
    attention_result_switch = bell_draw(streams_of[6], (MIX, TOKENS), 1.0, 6.0, ((0, 4), (1, 8)))
    fading_bias_vector = draw_fading_bias_vector(jax.random.fold_in(streams_of[15], 71), 0)
    surplus_forgetting = draw_surplus_forgetting(jax.random.fold_in(streams_of[15], 71), 0)
    per_group_scaler = jnp.clip(1.0 + 0.18 * jax.random.normal(streams_of[9], (MIX,), jnp.float32), 0.1, 1.9)
    attention_result_matrix = bell_draw(streams_of[10], (MIX, D), MIX ** -0.5, 0.125, ((0, 4),))
    dense_block_scaler = jnp.clip(1.0 + 0.18 * jax.random.normal(streams_of[11], (D,), jnp.float32), 0.1, 1.9)
    switching_matrix = bell_draw(streams_of[12], (D, FF), D ** -0.5, 0.125, ((0, 8), (1, 4)))
    expanding_matrix = bell_draw(streams_of[13], (D, FF), D ** -0.5, 0.125, ((0, 8), (1, 4)))
    contracting_matrix = bell_draw(streams_of[14], (FF, D), FF ** -0.5, 0.078125, ((0, 4), (1, 8)))
    return dict(residual_matrix=residual_matrix, query_vectors=query_vectors, lookup_vectors=lookup_vectors, payload_vectors=payload_vectors, fading_dependent_term=fading_dependent_term, step_size_preactivation=step_size_preactivation, attention_result_switch=attention_result_switch, fading_bias_vector=fading_bias_vector, surplus_forgetting=surplus_forgetting, per_group_scaler=per_group_scaler, attention_result_matrix=attention_result_matrix, dense_block_scaler=dense_block_scaler, switching_matrix=switching_matrix, expanding_matrix=expanding_matrix, contracting_matrix=contracting_matrix)


norm_eps = 1e-06
group_eps = 0.00064
key_eps = 1e-06
highest = lax.Precision.HIGHEST

def per_token(source):
    return source.astype(jnp.float32).reshape(HEADS, HEAD, TOKENS).transpose(2, 0, 1)

def reference(residual_matrix, query_vectors, lookup_vectors, payload_vectors, fading_dependent_term, step_size_preactivation, attention_result_switch, fading_bias_vector, surplus_forgetting, per_group_scaler, attention_result_matrix, dense_block_scaler, switching_matrix, expanding_matrix, contracting_matrix):
    read_rows = per_token(query_vectors)
    key_rows = per_token(lookup_vectors)
    value_rows = per_token(payload_vectors)
    fading_preactivation = per_token(fading_dependent_term) + fading_bias_vector.reshape(HEADS, HEAD)[None]
    log_fading_factor = -jnp.exp(-jax.nn.softplus(-fading_preactivation) - 0.5) + surplus_forgetting.T[:, :, None]
    learn_rate = jax.nn.sigmoid(per_token(step_size_preactivation))
    unit_keys = key_rows * lax.rsqrt(lax.optimization_barrier(jnp.sum(key_rows * key_rows, axis=-1, keepdims=True)) + key_eps)
    scaled = key_rows * learn_rate
    removal = unit_keys * learn_rate

    def advance(carried, member):
        read_step, decay_step, unit_step, removal_step, key_step, value_step = member
        seen_part = jnp.einsum('hij,hj->hi', carried, unit_step, precision=highest)
        carried = carried * decay_step[:, None, :] - seen_part[:, :, None] * removal_step[:, None, :] + value_step[:, :, None] * key_step[:, None, :]
        return (carried, jnp.einsum('hij,hj->hi', carried, read_step, precision=highest))
    zero_state = jnp.zeros((HEADS, HEAD, HEAD), jnp.float32)
    _, outputs = lax.scan(advance, zero_state, (read_rows, jnp.exp(log_fading_factor), unit_keys, removal, scaled, value_rows))
    centred = outputs - lax.optimization_barrier(jnp.mean(outputs, axis=-1, keepdims=True))
    variance = lax.optimization_barrier(jnp.mean(centred * centred, axis=-1, keepdims=True))
    normed_heads = (centred * lax.rsqrt(variance + group_eps)).reshape(TOKENS, HEADS * HEAD)
    mixed_out = (normed_heads * per_group_scaler[None, :] * attention_result_switch.astype(jnp.float32).T).astype(jnp.bfloat16)
    middle = residual_matrix.astype(jnp.float32) + jnp.dot(mixed_out, attention_result_matrix, preferred_element_type=jnp.float32)
    normed = (middle * lax.rsqrt(lax.optimization_barrier(jnp.mean(middle * middle, axis=-1, keepdims=True)) + norm_eps) * dense_block_scaler).astype(jnp.bfloat16)
    gate_sum = jnp.dot(normed, switching_matrix, preferred_element_type=jnp.float32)
    up_sum = jnp.dot(normed, expanding_matrix, preferred_element_type=jnp.float32)
    hidden = (jax.nn.silu(gate_sum) * up_sum).astype(jnp.bfloat16)
    group_width = FF // N_TP

    def add_group(total_sum, group_index):
        piece_rows = lax.dynamic_slice_in_dim(hidden, group_index * group_width, group_width, 1)
        down_rows = lax.dynamic_slice_in_dim(contracting_matrix, group_index * group_width, group_width, 0)
        product = jnp.dot(piece_rows, down_rows, preferred_element_type=jnp.float32)
        rounded = lax.optimization_barrier(product.astype(jnp.bfloat16))
        return (total_sum + rounded.astype(jnp.float32), None)
    channel_out, _ = lax.scan(add_group, jnp.zeros((TOKENS, D), jnp.float32), jnp.arange(N_TP, dtype=jnp.int32))
    return (middle + channel_out).astype(jnp.bfloat16)
```

```python
import jax
import jax.numpy as jnp
from jax import lax
from jax.sharding import PartitionSpec as P

HEAD = 64
BLOCK = 64


norm_eps = 1e-06
group_eps = 0.00064
key_eps = 1e-06
highest = lax.Precision.HIGHEST


def shifted(x, axis, by):
    n = lax.axis_size(axis)
    return lax.ppermute(x, axis, [(i, (i + by) % n) for i in range(n)])


def paired(x):
    n = lax.axis_size("sp")
    return lax.ppermute(x, "sp", [(i, i ^ 1) for i in range(n)])


def around(first, second):
    n = lax.axis_size("sp")
    ring = n // 2
    half = ring // 2

    def hop(x, by):
        return lax.ppermute(x, "sp", [(i, (i + 2 * by) % n) for i in range(n)])

    out = [[None] * ring, [None] * ring]
    for place, piece in enumerate((first, second)):
        out[place][0] = piece
        up = down = piece
        for step in range(1, half):
            up = hop(up, 1)
            down = hop(down, -1)
            out[place][ring - step] = up
            out[place][step] = down
        if ring > 1:
            out[place][half] = hop(up, 1) if place == 0 else hop(down, -1)
    return out


def rolled(x, by):
    return lax.dynamic_slice_in_dim(jnp.concatenate([x, x], axis=1), by, x.shape[1], 1)


def carried_in(summary):
    n = lax.axis_size("sp")
    carry_map, carry_add = summary
    both = jnp.concatenate([carry_map, carry_add], axis=1).astype(jnp.bfloat16)
    width = carry_map.shape[1]
    state = jnp.zeros_like(carry_add)
    for back in range(n - 1, 0, -1):
        came = lax.ppermute(both, "sp", [(i, i + back) for i in range(n - back)])
        came = came.astype(jnp.float32)
        state = (
            jnp.einsum("hvk,hkj->hvj", state, came[:, :width], precision=highest)
            + came[:, width:]
        )
    return state


def by_blocks(source, attention_group_count, position_count):
    return (
        source.astype(jnp.float32)
        .reshape(attention_group_count, HEAD, position_count // BLOCK, BLOCK)
        .transpose(0, 2, 3, 1)
    )


def compose(earlier, latter):
    return (
        jnp.einsum("...ij,...jk->...ik", earlier[0], latter[0], precision=highest),
        jnp.einsum("...ij,...jk->...ik", earlier[1], latter[0], precision=highest) + latter[1],
    )


def unit_lower_solve(mutual, right_side):
    power = -mutual
    solved = right_side
    for level in range((BLOCK - 1).bit_length()):
        solved = solved + jnp.einsum("hbts,hbsn->hbtn", power, solved, precision=highest)
        if level + 1 < (BLOCK - 1).bit_length():
            power = jnp.einsum("hbts,hbsu->hbtu", power, power, precision=highest)
    return solved


def rms_rows(middle, dense_block_scaler):
    scale_rows = lax.rsqrt(jnp.mean(middle * middle, axis=-1, keepdims=True) + norm_eps)
    return (middle * scale_rows * dense_block_scaler).astype(jnp.bfloat16)


def local(
    residual_matrix,
    query_vectors,
    lookup_vectors,
    payload_vectors,
    fading_dependent_term,
    step_size_preactivation,
    attention_result_switch,
    fading_bias_vector,
    surplus_forgetting,
    per_group_scaler,
    attention_result_matrix,
    dense_block_scaler,
    switching_matrix,
    expanding_matrix,
    contracting_matrix,
):
    count_sp, count_tp = lax.axis_size("sp"), lax.axis_size("tp")
    parity = lax.axis_index("sp") % 2
    ring_place = lax.axis_index("sp") // 2
    units = switching_matrix.shape[1] // 2

    def part(x, which, axis):
        return lax.dynamic_slice_in_dim(x, which * units, units, axis)

    gate_pieces = around(
        part(switching_matrix, parity, 1), paired(part(switching_matrix, 1 - parity, 1))
    )
    up_pieces = around(
        part(expanding_matrix, parity, 1), paired(part(expanding_matrix, 1 - parity, 1))
    )
    down_pieces = around(
        part(contracting_matrix, parity, 0), part(contracting_matrix, 1 - parity, 0)
    )
    out_blocks = [attention_result_matrix] + [
        shifted(attention_result_matrix, "tp", by) for by in range(1, count_tp)
    ]
    attention_group_count = surplus_forgetting.shape[0]
    position_count = surplus_forgetting.shape[1]
    block_count = position_count // BLOCK
    read_rows = by_blocks(query_vectors, attention_group_count, position_count)
    key_rows = by_blocks(lookup_vectors, attention_group_count, position_count)
    value_rows = by_blocks(payload_vectors, attention_group_count, position_count)
    fading_preactivation = by_blocks(
        fading_dependent_term, attention_group_count, position_count
    ) + fading_bias_vector.reshape(attention_group_count, 1, 1, HEAD)
    log_fading_factor = -jnp.exp(
        -jax.nn.softplus(-fading_preactivation) - 0.5
    ) + surplus_forgetting.reshape(attention_group_count, block_count, BLOCK, 1)
    learn_rate = jax.nn.sigmoid(
        by_blocks(step_size_preactivation, attention_group_count, position_count)
    )
    unit_keys = key_rows * lax.rsqrt(jnp.sum(key_rows * key_rows, axis=-1, keepdims=True) + key_eps)
    scaled = key_rows * learn_rate
    removal = unit_keys * learn_rate
    cum_after = jnp.cumsum(log_fading_factor, axis=2)
    before = cum_after - log_fading_factor
    cum_final = cum_after[:, :, -1:, :]
    probe_keys = unit_keys * jnp.exp(before)
    removal_in = removal * jnp.exp(-cum_after)
    scaled_in = scaled * jnp.exp(-cum_after)
    reads_out = read_rows * jnp.exp(cum_after)
    position = jnp.arange(BLOCK)
    strict = position[:, None] > position[None, :]
    up_to = position[:, None] >= position[None, :]
    mutual = jnp.where(
        strict, jnp.einsum("hbtn,hbsn->hbts", probe_keys, removal_in, precision=highest), 0.0
    )
    through = jnp.where(
        strict, jnp.einsum("hbtn,hbsn->hbts", probe_keys, scaled_in, precision=highest), 0.0
    )
    right_side = jnp.concatenate(
        [probe_keys, jnp.einsum("hbts,hbsn->hbtn", through, value_rows, precision=highest)], axis=-1
    )
    solved = unit_lower_solve(mutual, right_side)
    basis_part = solved[..., :HEAD]
    offset = solved[..., HEAD:]
    removal_end = removal * jnp.exp(cum_final - cum_after)
    scaled_end = scaled * jnp.exp(cum_final - cum_after)
    carry_map = jnp.eye(HEAD, dtype=jnp.float32) * jnp.exp(cum_final) - jnp.einsum(
        "hbtk,hbtj->hbkj", basis_part, removal_end, precision=highest
    )
    carry_add = jnp.einsum(
        "hbtv,hbtj->hbvj", value_rows, scaled_end, precision=highest
    ) - jnp.einsum("hbtv,hbtj->hbvj", offset, removal_end, precision=highest)
    summary = (carry_map[:, 0], carry_add[:, 0])
    for block in range(1, block_count):
        summary = compose(summary, (carry_map[:, block], carry_add[:, block]))
    carried = carried_in(summary)
    starts = [carried]
    for block in range(block_count - 1):
        carried = (
            jnp.einsum("hvk,hkj->hvj", carried, carry_map[:, block], precision=highest)
            + carry_add[:, block]
        )
        starts.append(carried)
    starts = jnp.stack(starts, axis=1)
    removed = -jnp.einsum("hbtk,hbvk->hbtv", basis_part, starts, precision=highest) - offset
    reach_removal = jnp.where(
        up_to, jnp.einsum("hbtn,hbsn->hbts", reads_out, removal_in, precision=highest), 0.0
    )
    reach_value = jnp.where(
        up_to, jnp.einsum("hbtn,hbsn->hbts", reads_out, scaled_in, precision=highest), 0.0
    )
    outputs = (
        jnp.einsum("hbtk,hbvk->hbtv", reads_out, starts, precision=highest)
        + jnp.einsum("hbts,hbsv->hbtv", reach_removal, removed, precision=highest)
        + jnp.einsum("hbts,hbsv->hbtv", reach_value, value_rows, precision=highest)
    )
    centred = outputs - jnp.mean(outputs, axis=-1, keepdims=True)
    normed_heads = centred * lax.rsqrt(
        jnp.mean(centred * centred, axis=-1, keepdims=True) + group_eps
    )
    normed_heads = normed_heads.transpose(0, 3, 1, 2).reshape(
        attention_group_count * HEAD, position_count
    )
    mixed_out = (
        normed_heads * per_group_scaler[:, None] * attention_result_switch.astype(jnp.float32)
    ).astype(jnp.bfloat16)
    moved_rows = lax.all_to_all(mixed_out, "tp", split_axis=1, concat_axis=0, tiled=True)
    tp_place = lax.axis_index("tp")
    channels = attention_result_matrix.shape[0]
    middle = residual_matrix.astype(jnp.float32)
    for by in range(count_tp):
        owner = (tp_place - by + count_tp) % count_tp
        middle = middle + jnp.einsum(
            "ct,cd->td",
            lax.dynamic_slice_in_dim(moved_rows, owner * channels, channels, 0),
            out_blocks[by],
            preferred_element_type=jnp.float32,
        )
    normed = rms_rows(middle, dense_block_scaler)
    depth = switching_matrix.shape[0]
    rows = normed.shape[0]
    turned = rolled(normed, ring_place * 2 * depth).reshape(rows, count_sp // 2, 2, depth)
    flipped = jnp.flip(turned, axis=2)
    near = jnp.where(parity == 0, turned, flipped).reshape(rows, count_sp * depth)
    far = paired(jnp.where(parity == 0, flipped, turned).reshape(rows, count_sp * depth))

    def spread(x):
        return jnp.concatenate([x] + [shifted(x, "tp", by) for by in range(1, count_tp)], axis=0)

    def stacked(pieces):
        return jnp.concatenate([x for pair in zip(*pieces) for x in pair], axis=0)

    gate_weight, up_weight = stacked(gate_pieces), stacked(up_pieces)

    def units_of(x):
        gate_sum = jnp.dot(x, gate_weight, preferred_element_type=jnp.float32)
        up_sum = jnp.dot(x, up_weight, preferred_element_type=jnp.float32)
        return (jax.nn.silu(gate_sum) * up_sum).astype(jnp.bfloat16)

    near_units = units_of(spread(near))
    near_sent = paired(near_units)
    far_units = units_of(spread(far))
    far_sent = paired(far_units)
    down_own = jnp.concatenate(down_pieces[0], axis=1)
    down_other = jnp.concatenate(down_pieces[1], axis=1)

    def summed(own, other):
        product = (
            jnp.dot(own, down_own, preferred_element_type=jnp.float32)
            + jnp.dot(other, down_other, preferred_element_type=jnp.float32)
        ).astype(jnp.bfloat16)
        total = product[:rows].astype(jnp.float32)
        for by in range(1, count_tp):
            total = total + shifted(product[by * rows : (by + 1) * rows], "tp", -by).astype(
                jnp.float32
            )
        return total

    far_sum = paired(summed(far_units, near_sent).astype(jnp.bfloat16)).astype(jnp.float32)
    near_sum = summed(near_units, far_sent)
    near_cols = near_sum.reshape(rows, count_sp // 2, 1, depth)
    far_cols = far_sum.reshape(rows, count_sp // 2, 1, depth)
    columns = jnp.concatenate(
        [
            jnp.where(parity == 0, near_cols, far_cols),
            jnp.where(parity == 0, far_cols, near_cols),
        ],
        axis=2,
    ).reshape(rows, count_sp * depth)
    channel_out = rolled(columns, (count_sp // 2 - ring_place) % (count_sp // 2) * 2 * depth)
    return (middle + channel_out).astype(jnp.bfloat16)


def solution(mesh):
    placed = (
        P(("sp", "tp"), None),
        P("tp", "sp"),
        P("tp", "sp"),
        P("tp", "sp"),
        P("tp", "sp"),
        P("tp", "sp"),
        P("tp", "sp"),
        P("tp"),
        P("tp", "sp"),
        P("tp"),
        P("tp", None),
        P(),
        P("sp", "tp"),
        P("sp", "tp"),
        P("tp", "sp"),
    )
    return jax.shard_map(
        local, mesh=mesh, in_specs=placed, out_specs=P(("sp", "tp"), None), check_vma=False
    )
```

```python
import jax
import jax.numpy as jnp
from jax import lax
from jax.sharding import PartitionSpec as P

HEAD = 64
BLOCK = 64


norm_eps = 1e-06
group_eps = 0.00064
key_eps = 1e-06
highest = lax.Precision.HIGHEST
high = lax.Precision.HIGH


def shifted(x, axis, by):
    n = lax.axis_size(axis)
    return lax.ppermute(x, axis, [(i, (i + by) % n) for i in range(n)])


def paired(x):
    n = lax.axis_size("sp")
    return lax.ppermute(x, "sp", [(i, i ^ 1) for i in range(n)])


def around(first, second):
    n = lax.axis_size("sp")
    ring = n // 2
    half = ring // 2

    def hop(x, by):
        return lax.ppermute(x, "sp", [(i, (i + 2 * by) % n) for i in range(n)])

    out = [[None] * ring, [None] * ring]
    for place, piece in enumerate((first, second)):
        out[place][0] = piece
        up = down = piece
        for step in range(1, half):
            up = hop(up, 1)
            down = hop(down, -1)
            out[place][ring - step] = up
            out[place][step] = down
        if ring > 1:
            out[place][half] = hop(up, 1) if place == 0 else hop(down, -1)
    return out


def rolled(x, by):
    return lax.dynamic_slice_in_dim(jnp.concatenate([x, x], axis=1), by, x.shape[1], 1)


def carried_in(summary):
    n = lax.axis_size("sp")
    carry_map, carry_add = summary
    both = jnp.concatenate([carry_map, carry_add], axis=1).astype(jnp.bfloat16)
    width = carry_map.shape[1]
    state = jnp.zeros_like(carry_add)
    for back in range(n - 1, 0, -1):
        came = lax.ppermute(both, "sp", [(i, i + back) for i in range(n - back)])
        came = came.astype(jnp.float32)
        state = (
            jnp.einsum("hvk,hkj->hvj", state, came[:, :width], precision=high)
            + came[:, width:]
        )
    return state


def by_blocks(source, attention_group_count, position_count):
    return (
        source.astype(jnp.float32)
        .reshape(attention_group_count, HEAD, position_count // BLOCK, BLOCK)
        .transpose(0, 2, 3, 1)
    )


def compose(earlier, latter):
    return (
        jnp.einsum("...ij,...jk->...ik", earlier[0], latter[0], precision=high),
        jnp.einsum("...ij,...jk->...ik", earlier[1], latter[0], precision=high) + latter[1],
    )


def unit_lower_solve(mutual, right_side):
    power = -mutual
    solved = right_side
    for level in range((BLOCK - 1).bit_length()):
        solved = solved + jnp.einsum("hbts,hbsn->hbtn", power, solved, precision=highest)
        if level + 1 < (BLOCK - 1).bit_length():
            power = jnp.einsum("hbts,hbsu->hbtu", power, power, precision=highest)
    return solved


def rms_rows(middle, dense_block_scaler):
    scale_rows = lax.rsqrt(jnp.mean(middle * middle, axis=-1, keepdims=True) + norm_eps)
    return (middle * scale_rows * dense_block_scaler).astype(jnp.bfloat16)


def local(
    residual_matrix,
    query_vectors,
    lookup_vectors,
    payload_vectors,
    fading_dependent_term,
    step_size_preactivation,
    attention_result_switch,
    fading_bias_vector,
    surplus_forgetting,
    per_group_scaler,
    attention_result_matrix,
    dense_block_scaler,
    switching_matrix,
    expanding_matrix,
    contracting_matrix,
):
    count_sp, count_tp = lax.axis_size("sp"), lax.axis_size("tp")
    parity = lax.axis_index("sp") % 2
    ring_place = lax.axis_index("sp") // 2
    units = switching_matrix.shape[1] // 2

    def part(x, which, axis):
        return lax.dynamic_slice_in_dim(x, which * units, units, axis)

    gate_pieces = around(
        part(switching_matrix, parity, 1), paired(part(switching_matrix, 1 - parity, 1))
    )
    up_pieces = around(
        part(expanding_matrix, parity, 1), paired(part(expanding_matrix, 1 - parity, 1))
    )
    down_pieces = around(
        part(contracting_matrix, parity, 0), part(contracting_matrix, 1 - parity, 0)
    )
    attention_group_count = surplus_forgetting.shape[0]
    position_count = surplus_forgetting.shape[1]
    block_count = position_count // BLOCK
    read_rows = by_blocks(query_vectors, attention_group_count, position_count)
    key_rows = by_blocks(lookup_vectors, attention_group_count, position_count)
    value_rows = by_blocks(payload_vectors, attention_group_count, position_count)
    fading_preactivation = by_blocks(
        fading_dependent_term, attention_group_count, position_count
    ) + fading_bias_vector.reshape(attention_group_count, 1, 1, HEAD)
    log_fading_factor = -jnp.exp(
        -jax.nn.softplus(-fading_preactivation) - 0.5
    ) + surplus_forgetting.reshape(attention_group_count, block_count, BLOCK, 1)
    learn_rate = jax.nn.sigmoid(
        by_blocks(step_size_preactivation, attention_group_count, position_count)
    )
    unit_keys = key_rows * lax.rsqrt(jnp.sum(key_rows * key_rows, axis=-1, keepdims=True) + key_eps)
    scaled = key_rows * learn_rate
    removal = unit_keys * learn_rate
    cum_after = jnp.cumsum(log_fading_factor, axis=2)
    before = cum_after - log_fading_factor
    cum_final = cum_after[:, :, -1:, :]
    probe_keys = unit_keys * jnp.exp(before)
    removal_in = removal * jnp.exp(-cum_after)
    scaled_in = scaled * jnp.exp(-cum_after)
    reads_out = read_rows * jnp.exp(cum_after)
    position = jnp.arange(BLOCK)
    strict = position[:, None] > position[None, :]
    up_to = position[:, None] >= position[None, :]
    mutual = jnp.where(
        strict, jnp.einsum("hbtn,hbsn->hbts", probe_keys, removal_in, precision=high), 0.0
    )
    through = jnp.where(
        strict, jnp.einsum("hbtn,hbsn->hbts", probe_keys, scaled_in, precision=high), 0.0
    )
    right_side = jnp.concatenate(
        [probe_keys, jnp.einsum("hbts,hbsn->hbtn", through, value_rows, precision=high)], axis=-1
    )
    solved = unit_lower_solve(mutual, right_side)
    basis_part = solved[..., :HEAD]
    offset = solved[..., HEAD:]
    removal_end = removal * jnp.exp(cum_final - cum_after)
    scaled_end = scaled * jnp.exp(cum_final - cum_after)
    carry_map = jnp.eye(HEAD, dtype=jnp.float32) * jnp.exp(cum_final) - jnp.einsum(
        "hbtk,hbtj->hbkj", basis_part, removal_end, precision=high
    )
    carry_add = jnp.einsum(
        "hbtv,hbtj->hbvj", value_rows, scaled_end, precision=high
    ) - jnp.einsum("hbtv,hbtj->hbvj", offset, removal_end, precision=high)
    summary = (carry_map[:, 0], carry_add[:, 0])
    for block in range(1, block_count):
        summary = compose(summary, (carry_map[:, block], carry_add[:, block]))
    carried = carried_in(summary)
    starts = [carried]
    for block in range(block_count - 1):
        carried = (
            jnp.einsum("hvk,hkj->hvj", carried, carry_map[:, block], precision=high)
            + carry_add[:, block]
        )
        starts.append(carried)
    starts = jnp.stack(starts, axis=1)
    removed = -jnp.einsum("hbtk,hbvk->hbtv", basis_part, starts, precision=high) - offset
    reach_removal = jnp.where(
        up_to, jnp.einsum("hbtn,hbsn->hbts", reads_out, removal_in, precision=high), 0.0
    )
    reach_value = jnp.where(
        up_to, jnp.einsum("hbtn,hbsn->hbts", reads_out, scaled_in, precision=high), 0.0
    )
    outputs = (
        jnp.einsum("hbtk,hbvk->hbtv", reads_out, starts, precision=high)
        + jnp.einsum("hbts,hbsv->hbtv", reach_removal, removed, precision=high)
        + jnp.einsum("hbts,hbsv->hbtv", reach_value, value_rows, precision=high)
    )
    centred = outputs - jnp.mean(outputs, axis=-1, keepdims=True)
    normed_heads = centred * lax.rsqrt(
        jnp.mean(centred * centred, axis=-1, keepdims=True) + group_eps
    )
    normed_heads = normed_heads.transpose(0, 3, 1, 2).reshape(
        attention_group_count * HEAD, position_count
    )
    mixed_out = (
        normed_heads * per_group_scaler[:, None] * attention_result_switch.astype(jnp.float32)
    ).astype(jnp.bfloat16)
    tp_place = lax.axis_index("tp")
    rows = residual_matrix.shape[0]
    partial = jnp.einsum(
        "ct,cd->td", mixed_out, attention_result_matrix, preferred_element_type=jnp.float32
    )

    def rows_of(x, by):
        owner = (tp_place + by) % count_tp
        return lax.dynamic_slice_in_dim(x, owner * rows, rows, 0)

    sent = partial.astype(jnp.bfloat16)
    middle = residual_matrix.astype(jnp.float32) + rows_of(partial, 0)
    for by in range(1, count_tp):
        middle = middle + shifted(rows_of(sent, by), "tp", by).astype(jnp.float32)
    normed = rms_rows(middle, dense_block_scaler)
    depth = switching_matrix.shape[0]
    turned = rolled(normed, ring_place * 2 * depth).reshape(rows, count_sp // 2, 2, depth)
    flipped = jnp.flip(turned, axis=2)
    near = jnp.where(parity == 0, turned, flipped).reshape(rows, count_sp * depth)
    far = paired(jnp.where(parity == 0, flipped, turned).reshape(rows, count_sp * depth))

    def spread(x):
        return jnp.concatenate([x] + [shifted(x, "tp", by) for by in range(1, count_tp)], axis=0)

    def stacked(pieces):
        return jnp.concatenate([x for pair in zip(*pieces) for x in pair], axis=0)

    gate_weight, up_weight = stacked(gate_pieces), stacked(up_pieces)

    def units_of(x):
        gate_sum = jnp.dot(x, gate_weight, preferred_element_type=jnp.float32)
        up_sum = jnp.dot(x, up_weight, preferred_element_type=jnp.float32)
        return (jax.nn.silu(gate_sum) * up_sum).astype(jnp.bfloat16)

    near_units = units_of(spread(near))
    near_sent = paired(near_units)
    far_units = units_of(spread(far))
    far_sent = paired(far_units)
    down_own = jnp.concatenate(down_pieces[0], axis=1)
    down_other = jnp.concatenate(down_pieces[1], axis=1)

    def summed(own, other):
        product = (
            jnp.dot(own, down_own, preferred_element_type=jnp.float32)
            + jnp.dot(other, down_other, preferred_element_type=jnp.float32)
        ).astype(jnp.bfloat16)
        total = product[:rows].astype(jnp.float32)
        for by in range(1, count_tp):
            total = total + shifted(product[by * rows : (by + 1) * rows], "tp", -by).astype(
                jnp.float32
            )
        return total

    far_sum = paired(summed(far_units, near_sent).astype(jnp.bfloat16)).astype(jnp.float32)
    near_sum = summed(near_units, far_sent)
    near_cols = near_sum.reshape(rows, count_sp // 2, 1, depth)
    far_cols = far_sum.reshape(rows, count_sp // 2, 1, depth)
    columns = jnp.concatenate(
        [
            jnp.where(parity == 0, near_cols, far_cols),
            jnp.where(parity == 0, far_cols, near_cols),
        ],
        axis=2,
    ).reshape(rows, count_sp * depth)
    channel_out = rolled(columns, (count_sp // 2 - ring_place) % (count_sp // 2) * 2 * depth)
    return (middle + channel_out).astype(jnp.bfloat16)


def solution(mesh):
    placed = (
        P(("sp", "tp"), None),
        P("tp", "sp"),
        P("tp", "sp"),
        P("tp", "sp"),
        P("tp", "sp"),
        P("tp", "sp"),
        P("tp", "sp"),
        P("tp"),
        P("tp", "sp"),
        P("tp"),
        P("tp", None),
        P(),
        P("sp", "tp"),
        P("sp", "tp"),
        P("tp", "sp"),
    )


    return jax.shard_map(
        local, mesh=mesh, in_specs=placed, out_specs=P(("sp", "tp"), None), check_vma=False
    )
```
